32 devices in a mesh: ep: 4 (over y, x), tp: 8 (over z, core).
Axes of the slice: x: 2, y: 2, z: 4, core: 2. Of those that a mesh axis runs over, the one named last changes fastest.
Arguments:
- queries: bfloat16 [3072, 2048], P('ep', 'tp'), may hold values from -6 to 6
- keys: bfloat16 [3072, 512], P('ep'), may hold values from -6 to 6
- values: bfloat16 [3072, 512], P('ep'), may hold values from -6 to 6
- query_gain: float32 [128], replicated, may hold values from 1 to 4.5
- key_gain: float32 [128], replicated, may hold values from 1 to 4.5
- out_weight: bfloat16 [2048, 2048], P('tp'), may hold values from -0.75 to 0.75
- tokens_b: bfloat16 [1536, 2048], P('ep'), may hold values from -6 to 6
- norm_gain: float32 [2048], replicated, may hold values from 0.1 to 1.9
- routes: int32 [1536, 2], P('ep'), may hold values from 0 to 15, all different within a row; in each aligned block of 48 rows (0 to 47, 48 to 95, ...) at most 8 rows name the same one
- route_weight: float32 [1536, 2], P('ep'), may hold values from 0.2 to 1
- gate_weight: bfloat16 [16, 2048, 4096], P('ep', None, 'tp'), may hold values from -0.125 to 0.125
- up_weight: bfloat16 [16, 2048, 4096], P('ep', None, 'tp'), may hold values from -0.125 to 0.125
- down_weight: bfloat16 [16, 4096, 2048], P('ep', 'tp'), may hold values from -0.09375 to 0.09375
Outputs:
- mixed_out: bfloat16 [3072, 2048], P(('ep', 'tp'))
- expert_out: bfloat16 [1536, 2048], P(('ep', 'tp'))
The draws below stay inside these ranges and needn't reach their ends.
Inputs may be any that keep to these rules, and one draw needn't show every extreme that they name: `routes`: A row names 2 different experts. In each aligned block of 48 rows no expert is named more than 8 times, a bound that some block reaches.
All inputs are finite; a program needn't handle non-finite values.
Results may differ from the reference program's by a relative error of at most 0.019.
Values may be sent and summed in bfloat16 or wider, within the bound.
A program may use at most 128 MiB of HBM per device.

```python
import math
import jax
import jax.numpy as jnp
import numpy as np
from jax import lax

D = 2048
HD = 128
HQ = 16
KVH = 4
GROUP = 4
FF = 4096
EXPERTS = 16
TOPK = 2
GRID_W = 64
TOK_DEV = 48
CAP = 8
LEN = 3072
TOKB = 1536
N_TP = 8


def draw_queries(key, part):
    drawn = jax.random.normal(jax.random.fold_in(key, 11), (LEN, HQ, HD), jnp.float32)
    return jnp.clip(drawn, -6.0, 6.0).reshape(LEN, HQ * HD).astype(jnp.bfloat16)


def draw_keys(key, part):
    drawn = jax.random.normal(jax.random.fold_in(key, 12), (LEN, KVH, HD), jnp.float32)
    return jnp.clip(drawn, -6.0, 6.0).reshape(LEN, KVH * HD).astype(jnp.bfloat16)


def draw_query_gain(key, part):
    uniform_g = jax.random.uniform(jax.random.fold_in(key, 13), (HD,), jnp.float32, 1.0, 2.0)
    return uniform_g


def draw_key_gain(key, part):
    uniform_g = jax.random.uniform(jax.random.fold_in(key, 14), (HD,), jnp.float32, 1.0, 2.0)
    return uniform_g


def block_scale(key, dims, pieces, smallest, top_value):
    level, own = 1.0, jax.random.fold_in(key, 6)
    for position, shards_of in pieces:
        steps = jnp.exp(jax.random.uniform(jax.random.fold_in(own, position), (shards_of,), jnp.float32, smallest / len(pieces), top_value / len(pieces)))
        level = level * jnp.repeat(steps, dims[position] // shards_of).reshape([-1 if axis == position else 1 for axis in range(len(dims))])
    return level


def deal_out(rng, own, number, rows, count, top, most, lean):
    sequence = jax.random.permutation(rng, count)
    heavy_load, common = load_shares(count, rows * top, most, lean, True), load_shares(count, rows * top, most, lean, False)
    places = jnp.arange(count)

    def named(sizes, rotation):
        used = int((sizes > 0).sum())
        fixed = max(1, used // 4)
        moved = fixed + (places - fixed + rotation * (used - fixed)) % max(1, count - fixed)
        return jnp.zeros((count,), jnp.int32).at[sequence[jnp.where(places < fixed, places, moved)]].set(jnp.asarray(sizes, jnp.int32))

    sizes = jnp.where(number % 4 == 0, named(heavy_load, number // 4), named(common, number - number // 4 - 1))
    mixed = jax.random.permutation(jax.random.fold_in(own, 3), count)
    donor, sink = mixed[0:count // 2 * 2:2], mixed[1:count // 2 * 2:2]
    room = jnp.minimum(sizes[donor] - 1, most - sizes[sink]) // 2
    room = jnp.where((donor == sequence[0]) | (sink == sequence[0]) | (sizes[sink] == 0), 0, jnp.maximum(room, 0))
    moved = jax.random.randint(jax.random.fold_in(own, 4), (count // 2,), 0, 1 << 20) % (room + 1)
    sizes = sizes.at[donor].add(-moved).at[sink].add(moved)
    labels = jnp.searchsorted(jnp.cumsum(sizes), jnp.arange(rows * top), side="right").astype(jnp.int32)
    table = labels.reshape(top, rows).T
    table = table[jax.random.permutation(jax.random.fold_in(own, 1), rows)]
    rotation = jax.random.randint(jax.random.fold_in(own, 2), (rows, 1), 0, top)
    return jnp.take_along_axis(table, (jnp.arange(top)[None, :] + rotation) % top, axis=1)


def load_shares(amount, total, most, slope, full):
    weights = [(1 << 20) // math.isqrt(grade ** slope) + 1 for grade in range(1, amount + 1)]
    largest = most if full else min(most, max(-(-total // amount), total * weights[0] // sum(weights)))
    least = 1 if total - largest >= amount - 1 else 0
    counts, rest = [largest] + [least] * (amount - 1), total - largest - least * (amount - 1)
    while rest > 0:
        movable = [i for i in range(1, amount) if counts[i] < largest] or [i for i in range(1, amount) if counts[i] < most]
        pool, budget = sum([weights[i] for i in movable]), rest
        for i in movable:
            extra = min(most - counts[i], max(1, budget * weights[i] // pool), rest)
            counts[i] = counts[i] + extra
            rest = rest - extra
    return np.array(counts)


def noise(own_key, shape, deviation, limit, pieces=(), kind=jnp.bfloat16):
    entries = jax.random.normal(own_key, shape, jnp.float32) * deviation
    if len(pieces) > 0:
        entries = block_scale(own_key, shape, pieces, -0.22, 0.18) * entries
    return jnp.clip(entries, min=-limit, max=limit).astype(kind)


def setup_inputs(seed: int = 0) -> dict:
    arg_keys = jax.random.split(jax.random.key(seed), 14)
    queries = draw_queries(jax.random.fold_in(arg_keys[13], 71), 0)
    keys = draw_keys(jax.random.fold_in(arg_keys[13], 71), 0)
    values = noise(arg_keys[2], (LEN, KVH * HD), 1.0, 6.0, ((0, 4),))
    query_gain = draw_query_gain(jax.random.fold_in(arg_keys[13], 71), 0)
    key_gain = draw_key_gain(jax.random.fold_in(arg_keys[13], 71), 0)
    out_weight = noise(arg_keys[5], (HQ * HD, D), (HD // 2) ** -0.5, 0.75, ((0, 8),))
    tokens_b = noise(arg_keys[6], (TOKB, D), 1.0, 6.0, ((0, 4),))
    norm_gain = jnp.clip(1.0 + 0.18 * jax.random.normal(arg_keys[7], (D,), jnp.float32), 0.1, 1.9)
    routes_keys = jax.random.split(jax.random.fold_in(arg_keys[8], 1), TOKB // TOK_DEV)
    routes_turns = jax.random.permutation(jax.random.fold_in(arg_keys[8], 3), TOKB // TOK_DEV)
    routes = jax.vmap(lambda own, number: deal_out(jax.random.fold_in(arg_keys[8], 2), own, number, TOK_DEV, EXPERTS, TOPK, CAP, 1))(routes_keys, routes_turns).reshape((TOKB, TOPK))
    route_weight = jnp.clip(jnp.exp(math.log(1.0) - 1.609438 * jax.random.uniform(arg_keys[9], (TOKB, TOPK), jnp.float32) ** block_scale(arg_keys[9], (TOKB, TOPK), ((0, 4),), -0.2, 0.2)), 0.2, 1.0)
    gate_weight = noise(arg_keys[10], (EXPERTS, D, FF), D ** -0.5, 0.125, ((0, 4), (2, 8)))
    up_weight = noise(arg_keys[11], (EXPERTS, D, FF), D ** -0.5, 0.125, ((0, 4), (2, 8)))
    down_weight = noise(arg_keys[12], (EXPERTS, FF, D), FF ** -0.5, 0.09375, ((0, 4), (1, 8)))
    return dict(queries=queries, keys=keys, values=values, query_gain=query_gain, key_gain=key_gain, out_weight=out_weight, tokens_b=tokens_b, norm_gain=norm_gain, routes=routes, route_weight=route_weight, gate_weight=gate_weight, up_weight=up_weight, down_weight=down_weight)


EPS = 1e-06
THETA = 10000.0
q_block = 64

def rotate(field, positions):
    n_freq = HD // 4
    row_pos = (positions // GRID_W).astype(jnp.float32)
    col_pos = (positions % GRID_W).astype(jnp.float32)
    inverse = THETA ** (-jnp.arange(n_freq, dtype=jnp.float32) / n_freq)
    angles = jnp.stack([row_pos[:, None] * inverse, col_pos[:, None] * inverse], axis=1)
    cosine = jnp.cos(angles)[:, None]
    sine = jnp.sin(angles)[:, None]
    length, n_heads = (field.shape[0], field.shape[1])
    halves = field.reshape(length, n_heads, 2, 2, n_freq)
    leading = halves[..., 0, :]
    second = halves[..., 1, :]
    turned = jnp.stack([leading * cosine - second * sine, second * cosine + leading * sine], axis=-2)
    return turned.reshape(length, n_heads, HD)

def prepare(source, gain_vec, positions, n_heads):
    length = source.shape[0]
    field = source.astype(jnp.float32).reshape(length, n_heads, HD)
    field = field * lax.rsqrt(lax.optimization_barrier(jnp.mean(field * field, axis=-1, keepdims=True)) + EPS) * gain_vec.astype(jnp.float32)
    return rotate(field, positions).astype(jnp.bfloat16)

def attend_block(query_blk, key_t, value_h):
    scores = jnp.einsum('qkgd,skd->kgqs', query_blk.astype(jnp.float32), key_t.astype(jnp.float32)) * HD ** (-0.5)
    row_max = lax.optimization_barrier(jnp.max(scores, axis=-1, keepdims=True))
    weights = jnp.exp(scores - row_max)
    totals = lax.optimization_barrier(jnp.sum(weights, axis=-1, keepdims=True))
    rounded = lax.optimization_barrier(weights.astype(jnp.bfloat16))
    merged = jnp.einsum('kgqs,skd->kgqd', rounded.astype(jnp.float32), value_h.astype(jnp.float32)) / totals
    return jnp.transpose(merged, (2, 0, 1, 3)).reshape(query_blk.shape[0], HQ * HD).astype(jnp.bfloat16)

def reference(queries, keys, values, query_gain, key_gain, out_weight, tokens_b, norm_gain, routes, route_weight, gate_weight, up_weight, down_weight):
    positions = jnp.arange(LEN, dtype=jnp.int32)
    query_t = prepare(queries, query_gain, positions, HQ).reshape(LEN // q_block, q_block, KVH, GROUP, HD)
    key_t = prepare(keys, key_gain, positions, KVH)
    value_h = values.reshape(LEN, KVH, HD)
    attended = lax.map(lambda query_blk: attend_block(query_blk, key_t, value_h), query_t).reshape(LEN, HQ * HD)
    mixed_out = jnp.dot(attended, out_weight, preferred_element_type=jnp.float32).astype(jnp.bfloat16)
    n_tokens = tokens_b.shape[0]
    n_blocks = n_tokens // TOK_DEV
    field = tokens_b.astype(jnp.float32)
    normed = (field * lax.rsqrt(lax.optimization_barrier(jnp.mean(field * field, axis=-1, keepdims=True)) + EPS) * norm_gain.astype(jnp.float32)).astype(jnp.bfloat16)
    assigned = routes.reshape(n_blocks, TOK_DEV * TOPK)
    onehot = (assigned[:, :, None] == jnp.arange(EXPERTS, dtype=jnp.int32)[None, None, :]).astype(jnp.int32)
    slot_rank = lax.optimization_barrier(jnp.sum((jnp.cumsum(onehot, axis=1) - onehot) * onehot, axis=-1))
    block_ids = jnp.arange(n_blocks, dtype=jnp.int32)[:, None]
    flat_slot = ((assigned * n_blocks + block_ids) * CAP + slot_rank).reshape(-1).astype(jnp.int32)
    row_ids = (block_ids * TOK_DEV + jnp.arange(TOK_DEV * TOPK, dtype=jnp.int32)[None, :] // TOPK).reshape(-1).astype(jnp.int32)
    slot_table = jnp.full((EXPERTS * n_blocks * CAP,), n_tokens, jnp.int32).at[flat_slot].set(row_ids)
    padded = jnp.concatenate([normed, jnp.zeros((1, D), jnp.bfloat16)], axis=0)
    width_part = FF // N_TP

    def expert_rows(stacked):
        row_index, gate_w, up_w, down_w = stacked
        inputs = padded[row_index].astype(jnp.float32)
        gate_act = jnp.einsum('nd,dtf->tnf', inputs, gate_w.reshape(D, N_TP, width_part).astype(jnp.float32))
        up_act = jnp.einsum('nd,dtf->tnf', inputs, up_w.reshape(D, N_TP, width_part).astype(jnp.float32))
        hidden = lax.optimization_barrier((jax.nn.silu(gate_act) * up_act).astype(jnp.bfloat16))
        partial_value = jnp.einsum('tnf,tfd->tnd', hidden.astype(jnp.float32), down_w.reshape(N_TP, width_part, D).astype(jnp.float32))
        partial_value = lax.optimization_barrier(partial_value.astype(jnp.bfloat16))
        return lax.optimization_barrier(jnp.sum(partial_value.astype(jnp.float32), axis=0)).astype(jnp.bfloat16)
    results = lax.map(expert_rows, (slot_table.reshape(EXPERTS, n_blocks * CAP), gate_weight, up_weight, down_weight))
    picked = results.reshape(-1, D)[flat_slot].astype(jnp.float32).reshape(n_tokens, TOPK, D)
    shares = route_weight / lax.optimization_barrier(jnp.sum(route_weight, axis=-1, keepdims=True))
    expert_out = lax.optimization_barrier(jnp.sum(shares[:, :, None] * picked, axis=1)).astype(jnp.bfloat16)
    return (mixed_out, expert_out)
```

```python
import functools

import jax
import jax.numpy as jnp
from jax import lax
from jax.experimental import pallas as pl
from jax.experimental.pallas import tpu as pltpu
from jax.sharding import PartitionSpec as P

HD = 128
HQ = 16
KVH = 4
EXPERTS = 16
TOPK = 2
GRID_W = 64
CAP = 8
EPS = 1e-06
THETA = 10000.0
LOG2E = 1.4426950408889634
MESH = pl.DeviceIdType.MESH
BF = jnp.bfloat16
F32 = jnp.float32


def remote(src, dst, send, recv, device):
    return pltpu.make_async_remote_copy(
        src_ref=src,
        dst_ref=dst,
        send_sem=send,
        recv_sem=recv,
        device_id=device,
        device_id_type=MESH,
    )


def turned(x, gain, cosine, sine):
    x = x.astype(F32)
    x = x * lax.rsqrt(jnp.mean(x * x, axis=-1, keepdims=True) + EPS) * gain
    lane = lax.broadcasted_iota(jnp.int32, x.shape, 1)
    partner = jnp.where(lane % 64 < 32, pltpu.roll(x, HD - 32, 1), pltpu.roll(x, 32, 1))
    return (x * cosine + partner * sine).astype(BF)


def kernel(
    n_ep,
    n_tp,
    tq,
    q_ref,
    k_ref,
    v_ref,
    cos_ref,
    sin_ref,
    qg_ref,
    kg_ref,
    wo_ref,
    tok_ref,
    ng_ref,
    route_ref,
    share_ref,
    wg_hbm,
    wu_hbm,
    wd_hbm,
    mixed_ref,
    expert_ref,
    wg,
    wu,
    wd,
    kv,
    qn,
    att,
    apart,
    asib,
    azr,
    outb,
    arr,
    part,
    sib,
    ret,
    zs,
    zr,
    w_sem,
    kv_s,
    kv_r,
    kvf_s,
    kvf_r,
    d_s,
    d_r,
    df_s,
    df_r,
    do_s,
    do_r,
    a_s,
    a_r,
    az_s,
    az_r,
    p_s,
    p_r,
    r_s,
    r_r,
    z_s,
    z_r,
):
    ep = lax.axis_index("ep")
    tp = lax.axis_index("tp")
    core = lax.rem(tp, 2)
    z = tp // 2
    n_z = n_tp // 2
    other = 1 - core
    sibling = (ep, z * 2 + other)
    ep_peers = [lax.rem(ep + k, n_ep) for k in range(1, n_ep)]
    z_peers = [lax.rem(z + k, n_z) for k in range(1, n_z)]
    n_rows = k_ref.shape[0]
    heads = q_ref.shape[1] // HD
    depth = tok_ref.shape[1]
    n_local = wg.shape[0]
    slots = n_z * CAP
    block = tok_ref.shape[0] // n_tp
    out_rows = mixed_ref.shape[0]

    weights = []
    for i in range(n_local):
        for j, (src, dst) in enumerate(((wg_hbm, wg), (wu_hbm, wu), (wd_hbm, wd))):
            copy = pltpu.make_async_copy(src.at[i], dst.at[i], w_sem.at[j, i])
            copy.start()
            weights.append(copy)

    barrier = pltpu.get_barrier_semaphore()
    for device in [sibling] + [(p, tp) for p in ep_peers] + [(ep, w * 2 + core) for w in z_peers]:
        pl.semaphore_signal(barrier, inc=1, device_id=device, device_id_type=MESH)

    cosine, sine = cos_ref[...], sin_ref[...]
    kv[0, ep] = turned(k_ref[...], kg_ref[...], cosine, sine)
    kv[1, ep] = v_ref[...]
    pl.semaphore_wait(barrier, n_ep + n_z - 1)
    sends = []
    for p in ep_peers:
        copy = remote(kv.at[core, ep], kv.at[core, ep], kv_s.at[p], kv_r.at[ep], (p, tp))
        copy.start()
        sends.append(copy)

    half = n_z * block
    route = route_ref[...]
    e_iota = lax.broadcasted_iota(jnp.int32, (EXPERTS, half), 0)
    hot0 = (e_iota == route[0:1]).astype(F32)
    hot1 = (e_iota == route[1:2]).astype(F32)
    before = lax.broadcasted_iota(jnp.int32, (half, half), 0)
    after = lax.broadcasted_iota(jnp.int32, (half, half), 1)
    earlier = ((before < after) & (before // block == after // block)).astype(F32)
    count = jnp.dot(
        (hot0 + hot1).astype(BF), earlier.astype(BF), preferred_element_type=F32
    )
    rank0 = jnp.sum(hot0 * count, axis=0, keepdims=True).astype(jnp.int32)
    rank1 = jnp.sum(hot1 * count, axis=0, keepdims=True).astype(jnp.int32)
    base = lax.broadcasted_iota(jnp.int32, (1, half), 1) // block * CAP
    slot0 = route[0:1] * slots + base + rank0
    slot1 = route[1:2] * slots + base + rank1
    j_iota = lax.broadcasted_iota(jnp.int32, (EXPERTS * slots, half), 0)
    is0 = j_iota == slot0
    is1 = j_iota == slot1
    mat = (is0 | is1).astype(F32).astype(BF)
    field = jnp.concatenate(
        [
            tok_ref[pl.ds(pl.multiple_of((2 * w + core) * block, 16), block), :]
            for w in range(n_z)
        ],
        axis=0,
    ).astype(F32)
    normed = (
        field * lax.rsqrt(jnp.mean(field * field, axis=-1, keepdims=True) + EPS) * ng_ref[...]
    ).astype(BF)
    outb[...] = (
        jnp.dot(mat, normed, preferred_element_type=F32)
        .astype(BF)
        .reshape(n_ep, n_local, slots, depth)
    )
    for p in ep_peers:
        copy = remote(outb.at[p], arr.at[:, core, ep], d_s.at[p], d_r.at[ep], (p, tp))
        copy.start()
        sends.append(copy)
    arr[:, core, ep] = outb[ep]
    copy = remote(outb.at[ep], arr.at[:, core, ep], do_s, do_r, sibling)
    copy.start()
    sends.append(copy)

    for g in range(heads):
        qn[pl.ds(g * n_rows, n_rows), :] = turned(
            q_ref[:, g * HD : (g + 1) * HD], qg_ref[...], cosine, sine
        )

    for p in ep_peers:
        remote(kv.at[core, p], kv.at[core, p], kv_s.at[p], kv_r.at[p], (p, tp)).wait_recv()
        copy = remote(kv.at[core, p], kv.at[core, p], kvf_s.at[p], kvf_r.at[p], sibling)
        copy.start()
        sends.append(copy)
    for p in ep_peers:
        remote(kv.at[other, p], kv.at[other, p], kvf_s.at[p], kvf_r.at[p], sibling).wait_recv()

    factor = HD ** (-0.5) * LOG2E
    length = n_ep * n_rows

    def attend(i, carry):
        at = pl.multiple_of(i * tq, tq)
        scores = lax.dot_general(
            qn[pl.ds(at, tq), :],
            kv[0].reshape(length, HD),
            (((1,), (1,)), ((), ())),
            preferred_element_type=F32,
        )
        top = jnp.max(scores, axis=1, keepdims=True)
        weight = jnp.exp2((scores - top) * factor)
        total = jnp.sum(weight, axis=1, keepdims=True)
        merged = jnp.dot(
            weight.astype(BF), kv[1].reshape(length, HD), preferred_element_type=F32
        )
        att[pl.ds(at, tq), :] = (merged / total).astype(BF)
        return carry

    lax.fori_loop(0, heads * n_rows // tq, attend, 0)

    def projected(t):
        total = None
        for g in range(heads):
            piece = jnp.dot(
                att[pl.ds(pl.multiple_of(g * n_rows + t * out_rows, 16), out_rows), :],
                wo_ref[pl.ds(g * HD, HD), :],
                preferred_element_type=F32,
            )
            total = piece if total is None else total + piece
        return total

    for w in range(n_z):
        apart[w] = projected(2 * w + other).astype(BF)
        copy = remote(apart.at[w], asib.at[w], a_s.at[w], a_r.at[w], sibling)
        copy.start()
        sends.append(copy)
    for w in z_peers:
        own = projected(2 * w + core)
        remote(apart.at[w], asib.at[w], a_s.at[w], a_r.at[w], sibling).wait_recv()
        asib[w] = (own + asib[w].astype(F32)).astype(BF)
        copy = remote(
            asib.at[w], azr.at[z], az_s.at[w], az_r.at[z], (ep, w * 2 + core)
        )
        copy.start()
        sends.append(copy)
    remote(apart.at[z], asib.at[z], a_s.at[z], a_r.at[z], sibling).wait_recv()
    asib[z] = (projected(2 * z + core) + asib[z].astype(F32)).astype(BF)

    for p in ep_peers:
        remote(outb.at[p], arr.at[:, core, p], d_s.at[p], d_r.at[p], (p, tp)).wait_recv()
        copy = remote(arr.at[:, core, p], arr.at[:, core, p], df_s.at[p], df_r.at[p], sibling)
        copy.start()
        sends.append(copy)
    remote(outb.at[ep], arr.at[:, other, ep], do_s, do_r, sibling).wait_recv()
    for p in ep_peers:
        remote(
            arr.at[:, other, p], arr.at[:, other, p], df_s.at[p], df_r.at[p], sibling
        ).wait_recv()

    def give_back(i):
        remote(part.at[i, other], sib.at[i], p_s.at[i], p_r.at[i], sibling).wait_recv()
        sib[i] = (part[i, core].astype(F32) + sib[i].astype(F32)).astype(BF)
        for p in ep_peers:
            copy = remote(sib.at[i, p], ret.at[ep, i], r_s.at[i, p], r_r.at[i, ep], (p, tp))
            copy.start()
            sends.append(copy)
        ret[ep, i] = sib[i, ep]

    for i in range(n_local):
        for copy in weights[3 * i : 3 * i + 3]:
            copy.wait()
        x = arr[i].reshape(2 * n_ep * slots, depth)
        gate = jnp.dot(x, wg[i], preferred_element_type=F32)
        up = jnp.dot(x, wu[i], preferred_element_type=F32)
        hidden = (gate / (1.0 + jnp.exp(-gate)) * up).astype(BF)
        part[i] = (
            jnp.dot(hidden, wd[i], preferred_element_type=F32)
            .astype(BF)
            .reshape(2, n_ep, slots, depth)
        )
        copy = remote(part.at[i, other], sib.at[i], p_s.at[i], p_r.at[i], sibling)
        copy.start()
        sends.append(copy)
        if i > 0:
            give_back(i - 1)
    give_back(n_local - 1)

    share = share_ref[...]
    share = share / jnp.sum(share, axis=0, keepdims=True)
    comb = jnp.where(is0, share[0:1], 0.0) + jnp.where(is1, share[1:2], 0.0)
    high = comb.astype(BF)
    low = (comb - high.astype(F32)).astype(BF)
    both = jnp.concatenate([high, low], axis=1)
    for p in ep_peers:
        for i in range(n_local):
            remote(
                sib.at[i, p], ret.at[p, i], r_s.at[i, p], r_r.at[i, p], (p, tp)
            ).wait_recv()
    rows = lax.dot_general(
        both,
        ret[...].reshape(EXPERTS * slots, depth),
        (((0,), (0,)), ((), ())),
        preferred_element_type=F32,
    )
    rows = rows[:half] + rows[half:]
    zs[...] = rows.astype(BF).reshape(n_z, block, depth)
    for w in z_peers:
        copy = remote(zs.at[w], zr.at[z], z_s.at[w], z_r.at[z], (ep, w * 2 + core))
        copy.start()
        sends.append(copy)

    total = asib[z].astype(F32)
    for w in z_peers:
        remote(asib.at[w], azr.at[w], az_s.at[w], az_r.at[w], (ep, w * 2 + core)).wait_recv()
        total = total + azr[w].astype(F32)
    mixed_ref[...] = total.astype(BF)
    total = zs[z].astype(F32)
    for w in z_peers:
        remote(zs.at[w], zr.at[w], z_s.at[w], z_r.at[w], (ep, w * 2 + core)).wait_recv()
        total = total + zr[w].astype(F32)
    expert_ref[...] = total.astype(BF)
    for copy in sends:
        copy.wait_send()


def on_device(
    queries,
    keys,
    values,
    query_gain,
    key_gain,
    out_weight,
    tokens_b,
    norm_gain,
    routes,
    route_weight,
    gate_weight,
    up_weight,
    down_weight,
):
    n_ep, n_tp = lax.axis_size("ep"), lax.axis_size("tp")
    ep, tp = lax.axis_index("ep"), lax.axis_index("tp")
    n_z = n_tp // 2
    n_rows = queries.shape[0]
    heads = queries.shape[1] // HD
    depth = tokens_b.shape[1]
    local_rows = tokens_b.shape[0]
    block = local_rows // n_tp
    n_local, _, ff = gate_weight.shape
    slots = n_z * CAP
    length = n_rows * n_ep
    tq = n_rows
    while tq * length > 256 * 3072:
        tq //= 2

    positions = ep * n_rows + jnp.arange(n_rows, dtype=jnp.int32)
    lane = jnp.arange(HD, dtype=jnp.int32)
    n_freq = HD // 4
    inverse = THETA ** (-(lane % n_freq).astype(F32) / n_freq)
    along = jnp.where(lane[None] < HD // 2, positions[:, None] // GRID_W, positions[:, None] % GRID_W)
    angle = along.astype(F32) * inverse
    cosine = jnp.cos(angle)
    sine = jnp.sin(angle) * jnp.where(lane % (2 * n_freq) < n_freq, -1.0, 1.0)

    kv_index = tp * heads // (HQ // KVH)
    own_keys = lax.dynamic_slice_in_dim(keys, kv_index * HD, HD, 1)
    own_values = lax.dynamic_slice_in_dim(values, kv_index * HD, HD, 1)

    def mine(table):
        split = table.reshape(n_z, 2, block, TOPK)
        own = lax.dynamic_index_in_dim(split, lax.rem(tp, 2), 1, keepdims=False)
        return own.reshape(n_z * block, TOPK).T

    vmem = pl.BlockSpec(memory_space=pltpu.VMEM)
    hbm = pl.BlockSpec(memory_space=pl.ANY)
    dma = pltpu.SemaphoreType.DMA
    out_rows = n_rows // n_tp
    scratch = [
        pltpu.VMEM(gate_weight.shape, BF),
        pltpu.VMEM(up_weight.shape, BF),
        pltpu.VMEM(down_weight.shape, BF),
        pltpu.VMEM((2, n_ep, n_rows, HD), BF),
        pltpu.VMEM((heads * n_rows, HD), BF),
        pltpu.VMEM((heads * n_rows, HD), BF),
        pltpu.VMEM((n_z, out_rows, depth), BF),
        pltpu.VMEM((n_z, out_rows, depth), BF),
        pltpu.VMEM((n_z, out_rows, depth), BF),
        pltpu.VMEM((n_ep, n_local, slots, depth), BF),
        pltpu.VMEM((n_local, 2, n_ep, slots, depth), BF),
        pltpu.VMEM((n_local, 2, n_ep, slots, depth), BF),
        pltpu.VMEM((n_local, n_ep, slots, depth), BF),
        pltpu.VMEM((n_ep, n_local, slots, depth), BF),
        pltpu.VMEM((n_z, block, depth), BF),
        pltpu.VMEM((n_z, block, depth), BF),
        dma((3, n_local)),
        dma((n_ep,)),
        dma((n_ep,)),
        dma((n_ep,)),
        dma((n_ep,)),
        dma((n_ep,)),
        dma((n_ep,)),
        dma((n_ep,)),
        dma((n_ep,)),
        dma,
        dma,
        dma((n_z,)),
        dma((n_z,)),
        dma((n_z,)),
        dma((n_z,)),
        dma((n_local,)),
        dma((n_local,)),
        dma((n_local, n_ep)),
        dma((n_local, n_ep)),
        dma((n_z,)),
        dma((n_z,)),
    ]
    return tuple(
        pl.pallas_call(
            functools.partial(kernel, n_ep, n_tp, tq),
            out_shape=(
                jax.ShapeDtypeStruct((out_rows, out_weight.shape[1]), BF),
                jax.ShapeDtypeStruct((block, depth), BF),
            ),
            in_specs=[vmem] * 12 + [hbm] * 3,
            out_specs=(vmem, vmem),
            scratch_shapes=scratch,
            compiler_params=pltpu.CompilerParams(
                collective_id=0, has_side_effects=True, vmem_limit_bytes=67043328
            ),
        )(
            queries,
            own_keys,
            own_values,
            cosine,
            sine,
            query_gain[None],
            key_gain[None],
            out_weight,
            tokens_b,
            norm_gain[None],
            mine(routes),
            mine(route_weight),
            gate_weight,
            up_weight,
            down_weight,
        )
    )


def solution(mesh):
    placed = (
        P("ep", "tp"),
        P("ep", None),
        P("ep", None),
        P(),
        P(),
        P("tp", None),
        P("ep", None),
        P(),
        P("ep", None),
        P("ep", None),
        P("ep", None, "tp"),
        P("ep", None, "tp"),
        P("ep", "tp", None),
    )
    return jax.shard_map(
        on_device,
        mesh=mesh,
        in_specs=placed,
        out_specs=(P(("ep", "tp"), None), P(("ep", "tp"), None)),
        check_vma=False,
    )
```
